32 devices in a mesh: grp: 2 (over y), st: 4 (over z), tp: 4 (over x, core).
Axes of the slice: x: 2, y: 2, z: 4, core: 2. Of those that a mesh axis runs over, the one named last changes fastest.
Arguments:
- tokens: bfloat16 [4096, 2048], P(('grp', 'st'), 'tp'), parts along dimension 0, may hold values from -180 to 180
- ret_query: bfloat16 [4096, 1024], P(('grp', 'st'), 'tp'), parts along dimension 0, may hold values from -6 to 6
- ret_key: bfloat16 [4096, 1024], P(('grp', 'st'), 'tp'), parts along dimension 0, may hold values from -6 to 6
- ret_value: bfloat16 [4096, 1024], P(('grp', 'st'), 'tp'), parts along dimension 0, may hold values from -6 to 6
- w_query: bfloat16 [2048, 2048], P(None, 'tp'), may hold values from -0.125 to 0.125
- w_key: bfloat16 [2048, 2048], P(None, 'tp'), may hold values from -0.125 to 0.125
- w_value: bfloat16 [2048, 2048], P(None, 'tp'), may hold values from -0.125 to 0.125
- w_gate: bfloat16 [2048, 4], replicated, may hold values from -0.125 to 0.125
- store: bfloat16 [24, 128, 2048], P('st'), may hold values from -6 to 6
- passage_ids: int32 [64, 4], P(('grp', 'st')), parts along dimension 0, may hold values from 0 to 23, as said below
Outputs:
- blended: bfloat16 [4096, 3072], P(('grp', 'st'), 'tp'), parts along dimension 0
The draws below stay inside these ranges and needn't reach their ends.
There are 2 independent parts, one for each index of `grp`. The reference program is written for one: setup_inputs(seed, part) draws one part's arguments, and reference() takes and returns one part's arrays. A program takes and returns all parts, laid end to end along the dimension named above; an argument that names none is the same for every part. Nothing has to cross between parts.
Inputs may be any that keep to these rules, and one draw needn't show every extreme that they name: `passage_ids`: passage p lies on index p // 6 of st. The 8 rows of one device name passages of any one index of st at most 16 times in all, and those of some index exactly 16 times.
All inputs are finite; a program needn't handle non-finite values.
Results may differ from the reference program's by a relative error of at most 0.0094.
Values may be sent and summed in bfloat16 or wider, within the bound.
A program may use at most 128 MiB of HBM per device.

```python
import jax
import jax.numpy as jnp
from jax import lax

D = 2048
HEADS = 4
RET_DIM = 256
HEAD_DIM = 512
PROWS = 128
BLOCK = 64
NPB = 4
TOK_DEV = 512
PASS_DEV = 6
SEQ_LEN = 256
TOKENS = 2048
BLK_DEV = 8
NBLK = 32
PASSAGES = 24
CAP = 16
N_ST = 4


def draw_tokens(key, part):
    layout = (TOK_DEV * N_ST, D)
    values = 1.5 * jax.random.truncated_normal(jax.random.fold_in(key, 11), -6.0, 6.0, layout, jnp.float32)
    return values.astype(jnp.bfloat16)


def requests_for(subkey, device):
    entries = jnp.arange(N_ST * CAP, dtype=jnp.int32)
    owner_of = entries // CAP
    copy_of = entries % CAP
    full_owner = (device + jax.random.randint(jax.random.fold_in(subkey, 1), (), 0, N_ST // 2)) % N_ST
    before_owner = (device + N_ST - 1) % N_ST
    across_owner = (device + N_ST // 2) % N_ST
    forced = (owner_of == full_owner) | (copy_of == 0) & ((owner_of == before_owner) | (owner_of == across_owner))
    popular = jax.random.randint(jax.random.fold_in(subkey, 2), (N_ST,), 0, 131072)
    jitter = jax.random.randint(jax.random.fold_in(subkey, 3), (N_ST * CAP,), 0, 32768)
    priority = jnp.where(forced, 524288, jnp.take(popular, owner_of) + jitter) * 1024 + entries
    _, chosen = lax.top_k(priority, BLK_DEV * NPB)
    within = jax.random.randint(jax.random.fold_in(subkey, 4), (BLK_DEV * NPB,), 0, PASS_DEV)
    picked = jnp.take(owner_of, chosen) * PASS_DEV + within
    return jax.random.permutation(jax.random.fold_in(subkey, 5), picked)


def draw_passage_ids(key, part):
    subkeys = jax.random.split(jax.random.fold_in(key, 21), N_ST)
    picked = jax.vmap(requests_for)(subkeys, jnp.arange(N_ST, dtype=jnp.int32))
    return picked.reshape(N_ST * BLK_DEV, NPB).astype(jnp.int32)


def level_of(rng, dims, cuts, least, high):
    def one(position, parts):
        steps = jax.random.uniform(jax.random.fold_in(jax.random.fold_in(rng, 6), position), (parts,), jnp.float32, least / len(cuts), high / len(cuts))
        return jnp.repeat(jnp.exp(steps), dims[position] // parts).reshape((-1,) + (1,) * (len(dims) - position - 1))

    gain = one(*cuts[0])
    for cut in cuts[1:]:
        gain = gain * one(*cut)
    return gain


def gaussian(own_key, extent, width, limit, shards=(), kind=jnp.bfloat16):
    gain = level_of(own_key, extent, shards, -0.22, 0.18) if shards else 1.0
    values = jax.random.normal(own_key, extent, jnp.float32) * width * gain
    return jnp.minimum(jnp.maximum(values, -limit), limit).astype(kind)


def setup_inputs(seed: int = 0, part: int = 0) -> dict:
    seeds = jax.random.split(jax.random.key(seed), 11)
    part_keys = jax.random.split(jax.random.fold_in(seeds[10], part), 11)
    return {
        "tokens": draw_tokens(jax.random.fold_in(jax.random.fold_in(seeds[10], part), 71), part),
        "ret_query": gaussian(part_keys[1], (TOKENS, HEADS * RET_DIM), 1.0, 6.0, ((0, 4), (1, 4))),
        "ret_key": gaussian(part_keys[2], (TOKENS, HEADS * RET_DIM), 1.0, 6.0, ((0, 4), (1, 4))),
        "ret_value": gaussian(part_keys[3], (TOKENS, HEADS * RET_DIM), 1.0, 6.0, ((0, 4), (1, 4))),
        "w_query": gaussian(seeds[4], (D, HEADS * HEAD_DIM), D ** -0.5, 0.125, ((1, 4),)),
        "w_key": gaussian(seeds[5], (D, HEADS * HEAD_DIM), D ** -0.5, 0.125, ((1, 4),)),
        "w_value": gaussian(seeds[6], (D, HEADS * HEAD_DIM), D ** -0.5, 0.125, ((1, 4),)),
        "w_gate": gaussian(seeds[7], (D, HEADS), D ** -0.5, 0.125),
        "store": gaussian(seeds[8], (PASSAGES, PROWS, D), 1.0, 6.0, ((0, 4),)),
        "passage_ids": draw_passage_ids(jax.random.fold_in(jax.random.fold_in(seeds[10], part), 71), part),
    }


ROTARY_BASE = 10000.0
NORM_EPS = 1e-05

def rounded(values):
    return lax.optimization_barrier(values.astype(jnp.bfloat16)).astype(jnp.float32)

def rotate(values, positions):
    halfway = values.shape[-1] // 2
    inverse = ROTARY_BASE ** (-jnp.arange(halfway, dtype=jnp.float32) / halfway)
    angles = positions.astype(jnp.float32)[:, None, None] * inverse
    cosines, sines = (jnp.cos(angles), jnp.sin(angles))
    leading, trailing = (values[..., :halfway], values[..., halfway:])
    return jnp.concatenate([leading * cosines - trailing * sines, leading * sines + trailing * cosines], axis=-1)

def retain_all(query_rows, key_rows, value_rows):
    layout = (TOKENS // SEQ_LEN, SEQ_LEN, HEADS, RET_DIM)
    places = jnp.arange(SEQ_LEN, dtype=jnp.int32)
    rot_query = rounded(rotate(query_rows.reshape(layout).astype(jnp.float32), places))
    rot_key = rounded(rotate(key_rows.reshape(layout).astype(jnp.float32), places) * RET_DIM ** (-0.5))
    head_number = jnp.arange(HEADS, dtype=jnp.float32)
    log_gamma = jnp.log1p(-jnp.exp2(-5.0 - head_number))
    offsets = (places[:, None] - places[None, :]).astype(jnp.float32)
    decays = jnp.where(offsets[None] >= 0.0, jnp.exp(log_gamma[:, None, None] * jnp.maximum(offsets, 0.0)[None]), 0.0)
    scores = jnp.einsum('sigd,sjgd->sgij', rot_query, rot_key)
    weights = rounded(scores * decays[None])
    output = jnp.einsum('sgij,sjge->sige', weights, value_rows.reshape(layout).astype(jnp.float32))
    centred = output - lax.optimization_barrier(jnp.mean(output, -1, keepdims=True))
    normed = centred * lax.rsqrt(lax.optimization_barrier(jnp.mean(centred * centred, -1, keepdims=True)) + NORM_EPS)
    return normed.astype(jnp.bfloat16).reshape(TOKENS, HEADS, RET_DIM)

def reference(tokens, ret_query, ret_key, ret_value, w_query, w_key, w_value, w_gate, store, passage_ids):
    retained = retain_all(ret_query, ret_key, ret_value)
    queries = jnp.dot(tokens, w_query, preferred_element_type=jnp.float32).astype(jnp.bfloat16)
    gate_vals = jax.nn.sigmoid(jnp.dot(tokens, w_gate, preferred_element_type=jnp.float32))
    keys_all = jnp.dot(store, w_key, preferred_element_type=jnp.float32).astype(jnp.bfloat16)
    values_all = jnp.dot(store, w_value, preferred_element_type=jnp.float32).astype(jnp.bfloat16)

    def attend(inputs):
        query_block, id_row, gate_block = inputs
        key_sel = jnp.take(keys_all, id_row, axis=0).reshape(NPB, PROWS, HEADS, HEAD_DIM).astype(jnp.float32)
        value_sel = jnp.take(values_all, id_row, axis=0).reshape(NPB, PROWS, HEADS, HEAD_DIM).astype(jnp.float32)
        scores = jnp.einsum('thd,jrhd->jhtr', query_block.astype(jnp.float32), key_sel) * HEAD_DIM ** (-0.5)
        highest = lax.optimization_barrier(jnp.max(scores, -1))
        exponent = jnp.exp(scores - highest[..., None])
        totals = lax.optimization_barrier(jnp.sum(exponent, -1))
        weighted = rounded(jnp.einsum('jhtr,jrhd->jthd', rounded(exponent), value_sel))
        overall = lax.optimization_barrier(jnp.max(highest, 0))
        scales = jnp.exp(highest - overall[None])
        denominator = lax.optimization_barrier(jnp.sum(scales * totals, 0))
        numerator = lax.optimization_barrier(jnp.sum(jnp.transpose(scales, (0, 2, 1))[..., None] * weighted, 0))
        return (gate_block[..., None] * numerator / jnp.transpose(denominator)[..., None]).astype(jnp.bfloat16)
    retrieved = lax.map(attend, (queries.reshape(NBLK, BLOCK, HEADS, HEAD_DIM), passage_ids, gate_vals.reshape(NBLK, BLOCK, HEADS)))
    retrieved = retrieved.reshape(TOKENS, HEADS, HEAD_DIM)
    return jnp.concatenate([retained, retrieved], -1).reshape(TOKENS, HEADS * (RET_DIM + HEAD_DIM))
```

```python
import functools

import jax
import jax.numpy as jnp
from jax import lax
from jax.experimental import pallas as pl
from jax.experimental.pallas import tpu as pltpu
from jax.sharding import PartitionSpec as P

RET_DIM = 256
HEAD_DIM = 512
BLOCK = 64
NPB = 4
SEQ_LEN = 256


ROTARY_BASE = 10000.0
NORM_EPS = 1e-05


def rotate(values, positions):
    halfway = values.shape[-1] // 2
    inverse = ROTARY_BASE ** (-jnp.arange(halfway, dtype=jnp.float32) / halfway)
    angles = positions.astype(jnp.float32)[:, None, None] * inverse
    cosines, sines = (jnp.cos(angles), jnp.sin(angles))
    leading, trailing = (values[..., :halfway], values[..., halfway:])
    return jnp.concatenate(
        [leading * cosines - trailing * sines, leading * sines + trailing * cosines], axis=-1
    )


def retain(query_rows, key_rows, value_rows, head_start):
    token_count = query_rows.shape[0]
    groups = query_rows.shape[1] // RET_DIM
    layout = (token_count // SEQ_LEN, SEQ_LEN, groups, RET_DIM)
    places = jnp.arange(SEQ_LEN, dtype=jnp.int32)
    rot_query = rotate(query_rows.reshape(layout).astype(jnp.float32), places).astype(jnp.bfloat16)
    rot_key = (
        rotate(key_rows.reshape(layout).astype(jnp.float32), places) * RET_DIM ** (-0.5)
    ).astype(jnp.bfloat16)
    head_number = (head_start + jnp.arange(groups, dtype=jnp.int32)).astype(jnp.float32)
    log_gamma = jnp.log1p(-jnp.exp2(-5.0 - head_number))
    offsets = (places[:, None] - places[None, :]).astype(jnp.float32)
    decays = jnp.where(
        offsets[None] >= 0.0,
        jnp.exp(log_gamma[:, None, None] * jnp.maximum(offsets, 0.0)[None]),
        0.0,
    )
    scores = jnp.einsum("sigd,sjgd->sgij", rot_query, rot_key, preferred_element_type=jnp.float32)
    weights = (scores * decays[None]).astype(jnp.bfloat16)
    output = jnp.einsum(
        "sgij,sjge->sige", weights, value_rows.reshape(layout), preferred_element_type=jnp.float32
    )
    centred = output - jnp.mean(output, -1, keepdims=True)
    normed = centred * lax.rsqrt(jnp.mean(centred * centred, -1, keepdims=True) + NORM_EPS)
    return normed.astype(jnp.bfloat16).reshape(token_count, groups, RET_DIM)


def partial_attend(query_block, kv_rows, head_width):
    leading = kv_rows.shape[:-2]
    groups = query_block.shape[-2]
    split_shape = leading + (kv_rows.shape[-2], groups, HEAD_DIM)
    key_part = kv_rows[..., :head_width].reshape(split_shape)
    value_part = kv_rows[..., head_width:].reshape(split_shape)
    scores = jnp.einsum(
        "...tgd,...rgd->...gtr", query_block, key_part, preferred_element_type=jnp.float32
    ) * HEAD_DIM ** (-0.5)
    highest = jnp.max(scores, -1)
    exponent = jnp.exp(scores - highest[..., None])
    totals = jnp.sum(exponent, -1)
    weighted = jnp.einsum(
        "...gtr,...rgd->...tgd",
        exponent.astype(jnp.bfloat16),
        value_part,
        preferred_element_type=jnp.float32,
    )
    return (
        weighted.astype(jnp.bfloat16).reshape(leading + (query_block.shape[-3], head_width)),
        highest,
        totals,
    )


def combine(weighted, highest, totals, gate_vals):
    block_count, per_block, span_len, head_width = weighted.shape
    groups = highest.shape[2]
    overall = jnp.max(highest, 1, keepdims=True)
    scales = jnp.exp(highest - overall)
    denominator = jnp.sum(scales * totals, 1)
    pieces = (
        lax.optimization_barrier(weighted)
        .reshape(block_count, per_block, span_len, groups, head_width // groups)
        .astype(jnp.float32)
    )
    numerator = jnp.sum(jnp.transpose(scales, (0, 1, 3, 2))[..., None] * pieces, 1)
    gate_cols = gate_vals.reshape(block_count, span_len, groups)[..., None]
    result = gate_cols * numerator / jnp.transpose(denominator, (0, 2, 1))[..., None]
    return result.astype(jnp.bfloat16).reshape(block_count * span_len, groups, head_width // groups)


def body(
    tokens, ret_query, ret_key, ret_value, w_query, w_key, w_value, w_gate, store, passage_ids
):
    owners = lax.axis_size("st")
    head_rank = lax.axis_index("tp")
    groups = w_query.shape[1] // HEAD_DIM
    head_width = groups * HEAD_DIM
    token_count = tokens.shape[0]
    block_count = token_count // BLOCK
    retained = retain(ret_query, ret_key, ret_value, head_rank * groups)
    shard_cols = lax.all_gather(tokens, "tp", axis=1, tiled=True)
    query_sum = jnp.dot(shard_cols, w_query, preferred_element_type=jnp.float32)
    gate_sum = jnp.dot(shard_cols, w_gate, preferred_element_type=jnp.float32)
    gate_vals = jax.nn.sigmoid(lax.dynamic_slice_in_dim(gate_sum, head_rank * groups, groups, 1))
    query_blocks = query_sum.astype(jnp.bfloat16).reshape(block_count, BLOCK, groups, HEAD_DIM)
    kv_own = jnp.concatenate(
        [
            jnp.dot(store, w_key, preferred_element_type=jnp.float32).astype(jnp.bfloat16),
            jnp.dot(store, w_value, preferred_element_type=jnp.float32).astype(jnp.bfloat16),
        ],
        axis=-1,
    )
    flat_ids = passage_ids.reshape(-1)
    requests = flat_ids.shape[0]
    capacity = max(2, 2 * requests // owners)
    owner_of = flat_ids // store.shape[0]
    within = flat_ids % store.shape[0]
    hit_table = (owner_of[:, None] == jnp.arange(owners, dtype=jnp.int32)[None, :]).astype(
        jnp.int32
    )
    earlier = (
        jnp.arange(requests, dtype=jnp.int32)[:, None]
        > jnp.arange(requests, dtype=jnp.int32)[None, :]
    ).astype(jnp.int32)
    slot_of = jnp.sum(jnp.dot(earlier, hit_table) * hit_table, 1)
    placed = (
        hit_table[:, :, None]
        * (slot_of[:, None] == jnp.arange(capacity, dtype=jnp.int32)[None, :]).astype(jnp.int32)[
            :, None, :
        ]
    )
    wanted = jnp.sum(placed * within[:, None, None], 0)
    fetch_at = owner_of * capacity + slot_of
    block_of = jnp.sum(placed * (jnp.arange(requests, dtype=jnp.int32) // NPB)[:, None, None], 0)
    outgoing = jnp.take(query_blocks, block_of, axis=0)
    incoming = lax.all_to_all(outgoing, "st", split_axis=0, concat_axis=0, tiled=True)
    indices = lax.all_to_all(wanted, "st", split_axis=0, concat_axis=0, tiled=True)
    weighted_here, highest_here, totals_here = partial_attend(
        incoming, jnp.take(kv_own, indices, axis=0), head_width
    )
    back_values = lax.all_to_all(weighted_here, "st", split_axis=0, concat_axis=0, tiled=True)
    returned = (
        back_values,
        lax.all_to_all(highest_here, "st", split_axis=0, concat_axis=0, tiled=True),
        lax.all_to_all(totals_here, "st", split_axis=0, concat_axis=0, tiled=True),
    )
    weighted = jnp.take(
        returned[0].reshape((owners * capacity,) + returned[0].shape[2:]), fetch_at, axis=0
    )
    weighted = weighted.reshape(block_count, NPB, BLOCK, head_width)
    highest = jnp.take(
        returned[1].reshape((owners * capacity,) + returned[1].shape[2:]), fetch_at, axis=0
    )
    highest = highest.reshape(block_count, NPB, groups, BLOCK)
    totals = jnp.take(
        returned[2].reshape((owners * capacity,) + returned[2].shape[2:]), fetch_at, axis=0
    )
    totals = totals.reshape(block_count, NPB, groups, BLOCK)
    retrieved = combine(weighted, highest, totals, gate_vals)
    return jnp.concatenate([retained, retrieved], -1).reshape(
        token_count, groups * (RET_DIM + HEAD_DIM)
    )

MESH = pl.DeviceIdType.MESH
NONE = -1e30
CHUNK = 128


def mixer_kernel(
    S, C, NP, PR,
    tok, wq, wg, keys, vals, bias, out,
    xg, qbuf, bin_, rin, sin_, rout, sout, gates,
    xsend, xrecv, bsend, brecv, qsl, qsr, qrecv, rsend, rrecv, ssend, srecv,
):
    s = lax.axis_index("st")
    tp = lax.axis_index("tp")
    core = lax.rem(tp, 2)
    sib = tp + 1 - 2 * core
    opp = lax.rem(tp + 2, 4)
    diag = lax.rem(sib + 2, 4)
    CH = qbuf.shape[2]
    depth = tok.shape[1]
    scale = HEAD_DIM ** (-0.5)

    barrier = pltpu.get_barrier_semaphore()
    for peer in (sib, opp):
        pl.semaphore_signal(barrier, inc=1, device_id={"tp": peer}, device_id_type=MESH)
    for k in range(1, S):
        pl.semaphore_signal(
            barrier, inc=1, device_id={"st": lax.rem(s + k, S)}, device_id_type=MESH
        )
    pl.semaphore_wait(barrier, S + 1)

    def rows(i):
        return pl.ds(pl.multiple_of(i * CH, CH), CH)

    def xcopy(kind, i):
        src = tok.at[rows(i)] if kind < 2 else xg.at[opp, rows(i)]
        slot = tp if kind < 2 else opp
        return pltpu.make_async_remote_copy(
            src_ref=src, dst_ref=xg.at[slot, rows(i)],
            send_sem=xsend.at[kind, i], recv_sem=xrecv.at[kind, i],
            device_id={"tp": opp if kind == 0 else sib}, device_id_type=MESH,
        )

    def bcopy(k):
        o = lax.rem(s + k, S)
        return pltpu.make_async_remote_copy(
            src_ref=bias.at[o], dst_ref=bin_.at[s],
            send_sem=bsend.at[k], recv_sem=brecv.at[k],
            device_id={"st": o}, device_id_type=MESH,
        )

    for i in range(C):
        xcopy(0, i).start()
        xcopy(1, i).start()
    for k in range(1, S):
        bcopy(k).start()
    bin_[s] = bias[s]

    def qcopy(u, i, right):
        return pltpu.make_async_remote_copy(
            src_ref=qbuf.at[u, i], dst_ref=qbuf.at[u, i],
            send_sem=(qsr if right else qsl).at[u, i], recv_sem=qrecv.at[u, i],
            device_id={"st": s + 1 if right else s - 1}, device_id_type=MESH,
        )

    def rcopies(u, i, left):
        if left:
            slot = u
            dev = s - 1
        else:
            slot = jnp.where(s + 1 == u, S, u)
            dev = s + 1
        return (
            pltpu.make_async_remote_copy(
                src_ref=rout.at[u, i], dst_ref=rin.at[slot, i],
                send_sem=rsend.at[u, i], recv_sem=rrecv.at[slot, i],
                device_id={"st": dev}, device_id_type=MESH,
            ),
            pltpu.make_async_remote_copy(
                src_ref=sout.at[u, i], dst_ref=sin_.at[slot, i],
                send_sem=ssend.at[u, i], recv_sem=srecv.at[slot, i],
                device_id={"st": dev}, device_id_type=MESH,
            ),
        )

    def recv_result(slot, i):
        pltpu.make_async_remote_copy(
            src_ref=rin.at[slot, i], dst_ref=rin.at[slot, i],
            send_sem=rsend.at[0, i], recv_sem=rrecv.at[slot, i],
            device_id={"st": lax.rem(s + 1, S)}, device_id_type=MESH,
        ).wait_recv()
        pltpu.make_async_remote_copy(
            src_ref=sin_.at[slot, i], dst_ref=sin_.at[slot, i],
            send_sem=ssend.at[0, i], recv_sem=srecv.at[slot, i],
            device_id={"st": lax.rem(s + 1, S)}, device_id_type=MESH,
        ).wait_recv()

    def project(i):
        xcopy(0, i).wait_recv()
        xcopy(2, i).start()
        acc = jnp.dot(
            tok[rows(i)], wq[pl.ds(pl.multiple_of(tp * depth, depth), depth)],
            preferred_element_type=jnp.float32,
        )
        gate = lax.dot_general(
            wg[tp], tok[rows(i)], (((1,), (1,)), ((), ())), preferred_element_type=jnp.float32
        )
        xcopy(1, i).wait_recv()
        for j in (opp, sib, diag):
            if j is diag:
                xcopy(2, i).wait_recv()
            part = xg[j, rows(i)]
            acc += jnp.dot(
                part, wq[pl.ds(pl.multiple_of(j * depth, depth), depth)],
                preferred_element_type=jnp.float32,
            )
            gate += lax.dot_general(
                wg[j], part, (((1,), (1,)), ((), ())), preferred_element_type=jnp.float32
            )
        gates[i] = jax.nn.sigmoid(gate[:8])
        qbuf[s, i] = acc.astype(jnp.bfloat16)

    def attend(u, i):
        sc = lax.dot_general(
            keys[...], qbuf[u, i], (((1,), (1,)), ((), ())), preferred_element_type=jnp.float32
        ) * scale
        sc = sc.reshape(NP, PR, CH) + bin_[u, i][:NP][:, None, :]
        top = jnp.max(jnp.max(sc, 0), 0, keepdims=True)
        ex = jnp.exp(sc - top[None])
        tot = jnp.sum(jnp.sum(ex, 0), 0, keepdims=True)
        part = jnp.dot(
            vals[...], ex.reshape(NP * PR, CH).astype(jnp.bfloat16),
            preferred_element_type=jnp.float32,
        )
        rout[u, i] = part.astype(jnp.bfloat16)
        sout[u, i] = jnp.concatenate(
            [jnp.broadcast_to(top, (4, CH)), jnp.broadcast_to(tot, (4, CH))], 0
        )

    def merge(u, i, slot):
        a, b = sout[u, i], sin_[slot, i]
        ma, ta, mb, tb = a[0:1], a[4:5], b[0:1], b[4:5]
        top = jnp.maximum(ma, mb)
        fa, fb = jnp.exp(ma - top), jnp.exp(mb - top)
        tot = fa * ta + fb * tb
        mixed = rout[u, i].astype(jnp.float32) * fa + rin[slot, i].astype(jnp.float32) * fb
        rout[u, i] = mixed.astype(jnp.bfloat16)
        sout[u, i] = jnp.concatenate(
            [jnp.broadcast_to(top, (4, CH)), jnp.broadcast_to(tot, (4, CH))], 0
        )

    for k in range(1, S):
        bcopy(k).wait_recv()

    def step(t, carry):
        def forward(u, c):
            k = jnp.abs(s - u)
            i = t - k

            @pl.when((u != s) & (i >= 0) & (i < C))
            def _():
                qcopy(u, i, True).wait_recv()

                @pl.when((u < s) & (s < S - 1))
                def _():
                    qcopy(u, i, True).start()

                @pl.when((u > s) & (s > 0))
                def _():
                    qcopy(u, i, False).start()

            return c

        lax.fori_loop(0, S, forward, 0)

        @pl.when(t < C)
        def _():
            project(t)

            @pl.when(s < S - 1)
            def _():
                qcopy(s, t, True).start()

            @pl.when(s > 0)
            def _():
                qcopy(s, t, False).start()

        def work(u, c):
            k = jnp.abs(s - u)
            i = t - k

            @pl.when((i >= 0) & (i < C))
            def _():
                attend(u, i)

            return c

        lax.fori_loop(0, S, work, 0)

        def back(u, c):
            k = jnp.abs(s - u)
            far = jnp.where(u < s, S - 1 - u, u)
            i = t - (2 * far - k)

            @pl.when((u != s) & (i >= 0) & (i < C))
            def _():
                @pl.when(k < far)
                def _():
                    recv_result(u, i)
                    merge(u, i, u)

                @pl.when(u < s)
                def _():
                    for copy in rcopies(u, i, True):
                        copy.start()

                @pl.when(u > s)
                def _():
                    for copy in rcopies(u, i, False):
                        copy.start()

            return c

        lax.fori_loop(0, S, back, 0)

        last = t - 2 * jnp.maximum(s, S - 1 - s)

        @pl.when((last >= 0) & (last < C))
        def _():
            @pl.when(s < S - 1)
            def _():
                recv_result(s, last)
                merge(s, last, s)

            @pl.when(s > 0)
            def _():
                recv_result(S, last)
                merge(s, last, S)

            ratio = gates[last][0:1] / sout[s, last][4:5]
            res = rout[s, last].astype(jnp.float32) * ratio
            out[rows(last)] = res.T.astype(jnp.bfloat16)

        return carry

    lax.fori_loop(0, C + 2 * (S - 1), step, 0)

    for i in range(C):
        for kind in range(3):
            xcopy(kind, i).wait_send()
    for k in range(1, S):
        bcopy(k).wait_send()

    def drain(n, c):
        u, i = n // C, n % C

        @pl.when((u <= s) & (s < S - 1))
        def _():
            qcopy(u, i, True).wait_send()

        @pl.when((u >= s) & (s > 0))
        def _():
            qcopy(u, i, False).wait_send()

        @pl.when(u < s)
        def _():
            for copy in rcopies(u, i, True):
                copy.wait_send()

        @pl.when(u > s)
        def _():
            for copy in rcopies(u, i, False):
                copy.wait_send()

        return c

    lax.fori_loop(0, S * C, drain, 0)


def fast_body(
    tokens, ret_query, ret_key, ret_value, w_query, w_key, w_value, w_gate, store, passage_ids
):
    S = lax.axis_size("st")
    ntp = lax.axis_size("tp")
    head = lax.axis_index("tp")
    T, depth = tokens.shape
    NP, PR, D = store.shape
    C = T // CHUNK
    per = CHUNK // BLOCK
    NPP = -(-NP // 8) * 8
    retained = retain(ret_query, ret_key, ret_value, head)
    flat = store.reshape(NP * PR, D)
    keys = jnp.dot(flat, w_key, preferred_element_type=jnp.float32).astype(jnp.bfloat16)
    vals = lax.dot_general(
        w_value, flat, (((0,), (1,)), ((), ())), preferred_element_type=jnp.float32
    ).astype(jnp.bfloat16)
    gate_row = lax.dynamic_slice_in_dim(w_gate, head, 1, 1).reshape(ntp, 1, depth)
    wg = jnp.broadcast_to(gate_row, (ntp, 16, depth))
    names = jnp.arange(S * NP, dtype=jnp.int32)
    counts = jnp.sum((passage_ids[:, :, None] == names).astype(jnp.float32), 1)
    bias = jnp.where(counts > 0, jnp.log(jnp.maximum(counts, 1.0)), NONE)
    bias = bias.reshape(C, per, S, NP).transpose(2, 0, 3, 1)
    bias = jnp.pad(bias, ((0, 0), (0, 0), (0, NPP - NP), (0, 0)), constant_values=NONE)
    bias = jnp.repeat(bias, BLOCK, axis=3)

    vm = pl.BlockSpec(memory_space=pltpu.VMEM)
    dma = pltpu.SemaphoreType.DMA
    retrieved = pl.pallas_call(
        functools.partial(mixer_kernel, S, C, NP, PR),
        out_shape=jax.ShapeDtypeStruct((T, HEAD_DIM), jnp.bfloat16),
        in_specs=[vm] * 6,
        out_specs=vm,
        scratch_shapes=[
            pltpu.VMEM((ntp, T, depth), jnp.bfloat16),
            pltpu.VMEM((S, C, CHUNK, HEAD_DIM), jnp.bfloat16),
            pltpu.VMEM((S, C, NPP, CHUNK), jnp.float32),
            pltpu.VMEM((S + 1, C, HEAD_DIM, CHUNK), jnp.bfloat16),
            pltpu.VMEM((S + 1, C, 8, CHUNK), jnp.float32),
            pltpu.VMEM((S, C, HEAD_DIM, CHUNK), jnp.bfloat16),
            pltpu.VMEM((S, C, 8, CHUNK), jnp.float32),
            pltpu.VMEM((C, 8, CHUNK), jnp.float32),
            dma((3, C)), dma((3, C)), dma((S,)), dma((S,)),
            dma((S, C)), dma((S, C)), dma((S, C)),
            dma((S, C)), dma((S + 1, C)), dma((S, C)), dma((S + 1, C)),
        ],
        compiler_params=pltpu.CompilerParams(
            collective_id=0, has_side_effects=True, vmem_limit_bytes=60 * 1024 * 1024
        ),
    )(tokens, w_query, wg, keys, vals, bias)
    return jnp.concatenate([retained.reshape(T, RET_DIM), retrieved], -1)


def solution(mesh):
    placed = (
        P(("grp", "st"), "tp"),
        P(("grp", "st"), "tp"),
        P(("grp", "st"), "tp"),
        P(("grp", "st"), "tp"),
        P(None, "tp"),
        P(None, "tp"),
        P(None, "tp"),
        P(),
        P("st", None, None),
        P(("grp", "st"), None),
    )

    def run(*args):
        heads = args[4].shape[1] // HEAD_DIM
        wide = 2 <= mesh.shape["st"] <= 8 and mesh.shape["tp"] == 4
        fast = wide and heads == mesh.shape["tp"] and args[7].shape[1] == heads
        return jax.shard_map(
            fast_body if fast else body,
            mesh=mesh, in_specs=placed, out_specs=P(("grp", "st"), "tp"), check_vma=False,
        )(*args)

    return run
```

```python
import functools

import jax
import jax.numpy as jnp
from jax import lax
from jax.experimental import pallas as pl
from jax.experimental.pallas import tpu as pltpu
from jax.sharding import PartitionSpec as P

RET_DIM = 256
HEAD_DIM = 512
BLOCK = 64
NPB = 4
SEQ_LEN = 256


ROTARY_BASE = 10000.0
NORM_EPS = 1e-05


def rotate(values, positions):
    halfway = values.shape[-1] // 2
    inverse = ROTARY_BASE ** (-jnp.arange(halfway, dtype=jnp.float32) / halfway)
    angles = positions.astype(jnp.float32)[:, None, None] * inverse
    cosines, sines = (jnp.cos(angles), jnp.sin(angles))
    leading, trailing = (values[..., :halfway], values[..., halfway:])
    return jnp.concatenate(
        [leading * cosines - trailing * sines, leading * sines + trailing * cosines], axis=-1
    )


def retain(query_rows, key_rows, value_rows, head_start):
    token_count = query_rows.shape[0]
    groups = query_rows.shape[1] // RET_DIM
    layout = (token_count // SEQ_LEN, SEQ_LEN, groups, RET_DIM)
    places = jnp.arange(SEQ_LEN, dtype=jnp.int32)
    rot_query = rotate(query_rows.reshape(layout).astype(jnp.float32), places).astype(jnp.bfloat16)
    rot_key = (
        rotate(key_rows.reshape(layout).astype(jnp.float32), places) * RET_DIM ** (-0.5)
    ).astype(jnp.bfloat16)
    head_number = (head_start + jnp.arange(groups, dtype=jnp.int32)).astype(jnp.float32)
    log_gamma = jnp.log1p(-jnp.exp2(-5.0 - head_number))
    offsets = (places[:, None] - places[None, :]).astype(jnp.float32)
    decays = jnp.where(
        offsets[None] >= 0.0,
        jnp.exp(log_gamma[:, None, None] * jnp.maximum(offsets, 0.0)[None]),
        0.0,
    )
    scores = jnp.einsum("sigd,sjgd->sgij", rot_query, rot_key, preferred_element_type=jnp.float32)
    weights = (scores * decays[None]).astype(jnp.bfloat16)
    output = jnp.einsum(
        "sgij,sjge->sige", weights, value_rows.reshape(layout), preferred_element_type=jnp.float32
    )
    centred = output - jnp.mean(output, -1, keepdims=True)
    normed = centred * lax.rsqrt(jnp.mean(centred * centred, -1, keepdims=True) + NORM_EPS)
    return normed.astype(jnp.bfloat16).reshape(token_count, groups, RET_DIM)


def partial_attend(query_block, kv_rows, head_width):
    leading = kv_rows.shape[:-2]
    groups = query_block.shape[-2]
    split_shape = leading + (kv_rows.shape[-2], groups, HEAD_DIM)
    key_part = kv_rows[..., :head_width].reshape(split_shape)
    value_part = kv_rows[..., head_width:].reshape(split_shape)
    scores = jnp.einsum(
        "...tgd,...rgd->...gtr", query_block, key_part, preferred_element_type=jnp.float32
    ) * HEAD_DIM ** (-0.5)
    highest = jnp.max(scores, -1)
    exponent = jnp.exp(scores - highest[..., None])
    totals = jnp.sum(exponent, -1)
    weighted = jnp.einsum(
        "...gtr,...rgd->...tgd",
        exponent.astype(jnp.bfloat16),
        value_part,
        preferred_element_type=jnp.float32,
    )
    return (
        weighted.astype(jnp.bfloat16).reshape(leading + (query_block.shape[-3], head_width)),
        highest,
        totals,
    )


def combine(weighted, highest, totals, gate_vals):
    block_count, per_block, span_len, head_width = weighted.shape
    groups = highest.shape[2]
    overall = jnp.max(highest, 1, keepdims=True)
    scales = jnp.exp(highest - overall)
    denominator = jnp.sum(scales * totals, 1)
    pieces = (
        lax.optimization_barrier(weighted)
        .reshape(block_count, per_block, span_len, groups, head_width // groups)
        .astype(jnp.float32)
    )
    numerator = jnp.sum(jnp.transpose(scales, (0, 1, 3, 2))[..., None] * pieces, 1)
    gate_cols = gate_vals.reshape(block_count, span_len, groups)[..., None]
    result = gate_cols * numerator / jnp.transpose(denominator, (0, 2, 1))[..., None]
    return result.astype(jnp.bfloat16).reshape(block_count * span_len, groups, head_width // groups)


def body(
    tokens, ret_query, ret_key, ret_value, w_query, w_key, w_value, w_gate, store, passage_ids
):
    owners = lax.axis_size("st")
    head_rank = lax.axis_index("tp")
    groups = w_query.shape[1] // HEAD_DIM
    head_width = groups * HEAD_DIM
    token_count = tokens.shape[0]
    block_count = token_count // BLOCK
    retained = retain(ret_query, ret_key, ret_value, head_rank * groups)
    shard_cols = lax.all_gather(tokens, "tp", axis=1, tiled=True)
    query_sum = jnp.dot(shard_cols, w_query, preferred_element_type=jnp.float32)
    gate_sum = jnp.dot(shard_cols, w_gate, preferred_element_type=jnp.float32)
    gate_vals = jax.nn.sigmoid(lax.dynamic_slice_in_dim(gate_sum, head_rank * groups, groups, 1))
    query_blocks = query_sum.astype(jnp.bfloat16).reshape(block_count, BLOCK, groups, HEAD_DIM)
    kv_own = jnp.concatenate(
        [
            jnp.dot(store, w_key, preferred_element_type=jnp.float32).astype(jnp.bfloat16),
            jnp.dot(store, w_value, preferred_element_type=jnp.float32).astype(jnp.bfloat16),
        ],
        axis=-1,
    )
    flat_ids = passage_ids.reshape(-1)
    requests = flat_ids.shape[0]
    capacity = max(2, 2 * requests // owners)
    owner_of = flat_ids // store.shape[0]
    within = flat_ids % store.shape[0]
    hit_table = (owner_of[:, None] == jnp.arange(owners, dtype=jnp.int32)[None, :]).astype(
        jnp.int32
    )
    earlier = (
        jnp.arange(requests, dtype=jnp.int32)[:, None]
        > jnp.arange(requests, dtype=jnp.int32)[None, :]
    ).astype(jnp.int32)
    slot_of = jnp.sum(jnp.dot(earlier, hit_table) * hit_table, 1)
    placed = (
        hit_table[:, :, None]
        * (slot_of[:, None] == jnp.arange(capacity, dtype=jnp.int32)[None, :]).astype(jnp.int32)[
            :, None, :
        ]
    )
    wanted = jnp.sum(placed * within[:, None, None], 0)
    fetch_at = owner_of * capacity + slot_of
    block_of = jnp.sum(placed * (jnp.arange(requests, dtype=jnp.int32) // NPB)[:, None, None], 0)
    outgoing = jnp.take(query_blocks, block_of, axis=0)
    incoming = lax.all_to_all(outgoing, "st", split_axis=0, concat_axis=0, tiled=True)
    indices = lax.all_to_all(wanted, "st", split_axis=0, concat_axis=0, tiled=True)
    weighted_here, highest_here, totals_here = partial_attend(
        incoming, jnp.take(kv_own, indices, axis=0), head_width
    )
    back_values = lax.all_to_all(weighted_here, "st", split_axis=0, concat_axis=0, tiled=True)
    returned = (
        back_values,
        lax.all_to_all(highest_here, "st", split_axis=0, concat_axis=0, tiled=True),
        lax.all_to_all(totals_here, "st", split_axis=0, concat_axis=0, tiled=True),
    )
    weighted = jnp.take(
        returned[0].reshape((owners * capacity,) + returned[0].shape[2:]), fetch_at, axis=0
    )
    weighted = weighted.reshape(block_count, NPB, BLOCK, head_width)
    highest = jnp.take(
        returned[1].reshape((owners * capacity,) + returned[1].shape[2:]), fetch_at, axis=0
    )
    highest = highest.reshape(block_count, NPB, groups, BLOCK)
    totals = jnp.take(
        returned[2].reshape((owners * capacity,) + returned[2].shape[2:]), fetch_at, axis=0
    )
    totals = totals.reshape(block_count, NPB, groups, BLOCK)
    retrieved = combine(weighted, highest, totals, gate_vals)
    return jnp.concatenate([retained, retrieved], -1).reshape(
        token_count, groups * (RET_DIM + HEAD_DIM)
    )

MESH = pl.DeviceIdType.MESH
NONE = -1e30
CHUNK = 128
LAG = 0


def mixer_kernel(
    S, C, NP, PR,
    tok_h, wq_h, wk_h, wv_h, store_h, rq_h, rk_h, rv_h, wg, bias, cosines, sines, decay, out,
    tok, wq, wk, wv, store, rq, rk, rv, keys, vals, lsem,
    xg, qbuf, bin_, rin, sin_, rout, sout, gates,
    xsend, xrecv, bsend, brecv, qsl, qsr, qrecv, rsend, rrecv, ssend, srecv,
):
    s = lax.axis_index("st")
    tp = lax.axis_index("tp")
    core = lax.rem(tp, 2)
    sib = tp + 1 - 2 * core
    opp = lax.rem(tp + 2, 4)
    diag = lax.rem(sib + 2, 4)
    CH = qbuf.shape[2]
    depth = tok.shape[1]
    scale = HEAD_DIM ** (-0.5)
    loads = [
        pltpu.make_async_copy(a, b, lsem.at[n])
        for n, (a, b) in enumerate((
            (tok_h, tok), (store_h, store), (wk_h, wk), (wq_h, wq), (wv_h, wv),
            (rq_h, rq), (rk_h, rk), (rv_h, rv),
        ))
    ]
    for load in loads:
        load.start()

    barrier = pltpu.get_barrier_semaphore()
    for peer in (sib, opp):
        pl.semaphore_signal(barrier, inc=1, device_id={"tp": peer}, device_id_type=MESH)
    for k in range(1, S):
        pl.semaphore_signal(
            barrier, inc=1, device_id={"st": lax.rem(s + k, S)}, device_id_type=MESH
        )
    pl.semaphore_wait(barrier, S + 1)
    loads[0].wait()

    def rows(i):
        return pl.ds(pl.multiple_of(i * CH, CH), CH)

    def xcopy(kind, i):
        src = tok.at[rows(i)] if kind < 2 else xg.at[opp, rows(i)]
        slot = tp if kind < 2 else opp
        return pltpu.make_async_remote_copy(
            src_ref=src, dst_ref=xg.at[slot, rows(i)],
            send_sem=xsend.at[kind, i], recv_sem=xrecv.at[kind, i],
            device_id={"tp": opp if kind == 0 else sib}, device_id_type=MESH,
        )

    def bcopy(k):
        o = lax.rem(s + k, S)
        return pltpu.make_async_remote_copy(
            src_ref=bias.at[o], dst_ref=bin_.at[s],
            send_sem=bsend.at[k], recv_sem=brecv.at[k],
            device_id={"st": o}, device_id_type=MESH,
        )

    for i in range(C):
        xcopy(0, i).start()
        xcopy(1, i).start()
    for k in range(1, S):
        bcopy(k).start()
    bin_[s] = bias[s]

    def qcopy(u, i, right):
        return pltpu.make_async_remote_copy(
            src_ref=qbuf.at[u, i], dst_ref=qbuf.at[u, i],
            send_sem=(qsr if right else qsl).at[u, i], recv_sem=qrecv.at[u, i],
            device_id={"st": s + 1 if right else s - 1}, device_id_type=MESH,
        )

    def rcopies(u, i, left):
        if left:
            slot = u
            dev = s - 1
        else:
            slot = jnp.where(s + 1 == u, S, u)
            dev = s + 1
        return (
            pltpu.make_async_remote_copy(
                src_ref=rout.at[u, i], dst_ref=rin.at[slot, i],
                send_sem=rsend.at[u, i], recv_sem=rrecv.at[slot, i],
                device_id={"st": dev}, device_id_type=MESH,
            ),
            pltpu.make_async_remote_copy(
                src_ref=sout.at[u, i], dst_ref=sin_.at[slot, i],
                send_sem=ssend.at[u, i], recv_sem=srecv.at[slot, i],
                device_id={"st": dev}, device_id_type=MESH,
            ),
        )

    def recv_result(slot, i):
        pltpu.make_async_remote_copy(
            src_ref=rin.at[slot, i], dst_ref=rin.at[slot, i],
            send_sem=rsend.at[0, i], recv_sem=rrecv.at[slot, i],
            device_id={"st": lax.rem(s + 1, S)}, device_id_type=MESH,
        ).wait_recv()
        pltpu.make_async_remote_copy(
            src_ref=sin_.at[slot, i], dst_ref=sin_.at[slot, i],
            send_sem=ssend.at[0, i], recv_sem=srecv.at[slot, i],
            device_id={"st": lax.rem(s + 1, S)}, device_id_type=MESH,
        ).wait_recv()

    def gate_part(j, part):
        cols = pl.ds(pl.multiple_of(j * depth, depth), depth)
        return lax.dot_general(
            wg[:, cols], part, (((1,), (1,)), ((), ())), preferred_element_type=jnp.float32
        )

    RB = 2 * PR if NP % 2 == 0 else PR

    def key_rows(n, c):
        r = pl.ds(pl.multiple_of(n * RB, RB), RB)
        keys[r] = jnp.dot(
            store[r], wk[...], preferred_element_type=jnp.float32
        ).astype(jnp.bfloat16)
        return c

    def value_rows(n, c):
        r = pl.ds(pl.multiple_of(n * RB, RB), RB)
        vals[:, r] = jnp.dot(
            store[r], wv[...], preferred_element_type=jnp.float32
        ).T.astype(jnp.bfloat16)
        return c

    def turned(ref, r, factor):
        half = RET_DIM // 2
        a = ref[r, :half].astype(jnp.float32)
        b = ref[r, half:].astype(jnp.float32)
        cs, sn = cosines[...], sines[...]
        both = jnp.concatenate([a * cs - b * sn, a * sn + b * cs], -1) * factor
        return both.astype(jnp.bfloat16)

    def retention(n):
        r = pl.ds(pl.multiple_of(n * SEQ_LEN, SEQ_LEN), SEQ_LEN)
        sc = lax.dot_general(
            turned(rq, r, 1.0), turned(rk, r, RET_DIM ** (-0.5)),
            (((1,), (1,)), ((), ())), preferred_element_type=jnp.float32,
        )
        raw = jnp.dot(
            (sc * decay[...]).astype(jnp.bfloat16), rv[r], preferred_element_type=jnp.float32
        )
        mid = raw - jnp.mean(raw, -1, keepdims=True)
        var = jnp.mean(mid * mid, -1, keepdims=True)
        out[r, :RET_DIM] = (mid * lax.rsqrt(var + NORM_EPS)).astype(jnp.bfloat16)

    def project(i):
        xcopy(0, i).wait_recv()
        xcopy(2, i).start()
        acc = jnp.dot(
            tok[rows(i)], wq[pl.ds(pl.multiple_of(tp * depth, depth), depth)],
            preferred_element_type=jnp.float32,
        )
        gate = gate_part(tp, tok[rows(i)])
        xcopy(1, i).wait_recv()
        for j in (opp, sib, diag):
            if j is diag:
                xcopy(2, i).wait_recv()
            part = xg[j, rows(i)]
            acc += jnp.dot(
                part, wq[pl.ds(pl.multiple_of(j * depth, depth), depth)],
                preferred_element_type=jnp.float32,
            )
            gate += gate_part(j, part)
        gates[i] = jax.nn.sigmoid(gate[:8])
        qbuf[s, i] = acc.astype(jnp.bfloat16)

    def attend(u, i):
        sc = lax.dot_general(
            keys[...], qbuf[u, i], (((1,), (1,)), ((), ())), preferred_element_type=jnp.float32
        ) * scale
        sc = sc.reshape(NP, PR, CH) + bin_[u, i][:NP][:, None, :]
        top = jnp.max(jnp.max(sc, 0), 0, keepdims=True)
        ex = jnp.exp(sc - top[None])
        tot = jnp.sum(jnp.sum(ex, 0), 0, keepdims=True)
        part = jnp.dot(
            vals[...], ex.reshape(NP * PR, CH).astype(jnp.bfloat16),
            preferred_element_type=jnp.float32,
        )
        rout[u, i] = part.astype(jnp.bfloat16)
        sout[u, i] = jnp.concatenate(
            [jnp.broadcast_to(top, (4, CH)), jnp.broadcast_to(tot, (4, CH))], 0
        )

    def merge(u, i, slot):
        a, b = sout[u, i], sin_[slot, i]
        ma, ta, mb, tb = a[0:1], a[4:5], b[0:1], b[4:5]
        top = jnp.maximum(ma, mb)
        fa, fb = jnp.exp(ma - top), jnp.exp(mb - top)
        tot = fa * ta + fb * tb
        mixed = rout[u, i].astype(jnp.float32) * fa + rin[slot, i].astype(jnp.float32) * fb
        rout[u, i] = mixed.astype(jnp.bfloat16)
        sout[u, i] = jnp.concatenate(
            [jnp.broadcast_to(top, (4, CH)), jnp.broadcast_to(tot, (4, CH))], 0
        )

    loads[1].wait()
    loads[2].wait()
    lax.fori_loop(0, NP * PR // RB, key_rows, 0)
    loads[3].wait()
    steps = C + 2 * (S - 1) + LAG
    seqs = tok.shape[0] // SEQ_LEN

    def step(t, carry):
        @pl.when(t < C)
        def _():
            project(t)

            @pl.when(s < S - 1)
            def _():
                qcopy(s, t, True).start()

            @pl.when(s > 0)
            def _():
                qcopy(s, t, False).start()

        @pl.when(t == 0)
        def _():
            loads[4].wait()
            lax.fori_loop(0, NP * PR // RB, value_rows, 0)
            for k in range(1, S):
                bcopy(k).wait_recv()

        def source(u, c):
            k = jnp.abs(s - u)
            i = t - k

            @pl.when((u != s) & (i >= 0) & (i < C))
            def _():
                qcopy(u, i, True).wait_recv()

                @pl.when((u < s) & (s < S - 1))
                def _():
                    qcopy(u, i, True).start()

                @pl.when((u > s) & (s > 0))
                def _():
                    qcopy(u, i, False).start()

            n = i - LAG

            @pl.when((n >= 0) & (n < C))
            def _():
                attend(u, n)

            far = jnp.where(u < s, S - 1 - u, u)
            m = t - (2 * far - k) - LAG

            @pl.when((u != s) & (m >= 0) & (m < C))
            def _():
                @pl.when(k < far)
                def _():
                    recv_result(u, m)
                    merge(u, m, u)

                @pl.when(u < s)
                def _():
                    for copy in rcopies(u, m, True):
                        copy.start()

                @pl.when(u > s)
                def _():
                    for copy in rcopies(u, m, False):
                        copy.start()

            return c

        lax.fori_loop(0, S, source, 0)

        first = steps - 1 - seqs

        @pl.when(t == first)
        def _():
            for load in loads[5:]:
                load.wait()

        @pl.when((t >= first) & (t < first + seqs))
        def _():
            retention(t - first)

        last = t - 2 * jnp.maximum(s, S - 1 - s) - LAG

        @pl.when((last >= 0) & (last < C))
        def _():
            @pl.when(s < S - 1)
            def _():
                recv_result(s, last)
                merge(s, last, s)

            @pl.when(s > 0)
            def _():
                recv_result(S, last)
                merge(s, last, S)

            ratio = gates[last, pl.ds(tp, 1)] / sout[s, last][4:5]
            res = rout[s, last].astype(jnp.float32) * ratio
            out[rows(last), RET_DIM:] = res.T.astype(jnp.bfloat16)

        return carry

    lax.fori_loop(0, steps, step, 0)

    for i in range(C):
        for kind in range(3):
            xcopy(kind, i).wait_send()
    for k in range(1, S):
        bcopy(k).wait_send()

    def drain(n, c):
        u, i = n // C, n % C

        @pl.when((u <= s) & (s < S - 1))
        def _():
            qcopy(u, i, True).wait_send()

        @pl.when((u >= s) & (s > 0))
        def _():
            qcopy(u, i, False).wait_send()

        @pl.when(u < s)
        def _():
            for copy in rcopies(u, i, True):
                copy.wait_send()

        @pl.when(u > s)
        def _():
            for copy in rcopies(u, i, False):
                copy.wait_send()

        return c

    lax.fori_loop(0, S * C, drain, 0)


def fast_body(
    tokens, ret_query, ret_key, ret_value, w_query, w_key, w_value, w_gate, store, passage_ids
):
    S = lax.axis_size("st")
    ntp = lax.axis_size("tp")
    head = lax.axis_index("tp")
    T, depth = tokens.shape
    NP, PR, D = store.shape
    C = T // CHUNK
    per = CHUNK // BLOCK
    NPP = -(-NP // 8) * 8
    heads = w_gate.shape[1]
    flat = store.reshape(NP * PR, D)
    wg = jnp.pad(w_gate.T, ((0, -heads % 16), (0, 0)))
    places = jnp.arange(SEQ_LEN, dtype=jnp.float32)
    half = RET_DIM // 2
    inverse = ROTARY_BASE ** (-jnp.arange(half, dtype=jnp.float32) / half)
    angles = places[:, None] * inverse
    log_gamma = jnp.log1p(-jnp.exp2(-5.0 - head.astype(jnp.float32)))
    offsets = places[:, None] - places[None, :]
    decay = jnp.where(offsets >= 0.0, jnp.exp(log_gamma * jnp.maximum(offsets, 0.0)), 0.0)
    names = jnp.arange(S * NP, dtype=jnp.int32)
    counts = jnp.sum((passage_ids[:, :, None] == names).astype(jnp.float32), 1)
    bias = jnp.where(counts > 0, jnp.log(jnp.maximum(counts, 1.0)), NONE)
    bias = bias.reshape(C, per, S, NP).transpose(2, 0, 3, 1)
    bias = jnp.pad(bias, ((0, 0), (0, 0), (0, NPP - NP), (0, 0)), constant_values=NONE)
    bias = jnp.repeat(bias, BLOCK, axis=3)

    vm = pl.BlockSpec(memory_space=pltpu.VMEM)
    hbm = pl.BlockSpec(memory_space=pl.ANY)
    bf = jnp.bfloat16
    dma = pltpu.SemaphoreType.DMA
    return pl.pallas_call(
        functools.partial(mixer_kernel, S, C, NP, PR),
        out_shape=jax.ShapeDtypeStruct((T, RET_DIM + HEAD_DIM), jnp.bfloat16),
        in_specs=[hbm] * 8 + [vm] * 5,
        out_specs=vm,
        scratch_shapes=[
            pltpu.VMEM((T, depth), bf),
            pltpu.VMEM(w_query.shape, bf), pltpu.VMEM(w_key.shape, bf),
            pltpu.VMEM(w_value.shape, bf), pltpu.VMEM(flat.shape, bf),
            pltpu.VMEM((T, RET_DIM), bf), pltpu.VMEM((T, RET_DIM), bf),
            pltpu.VMEM((T, RET_DIM), bf),
            pltpu.VMEM((NP * PR, HEAD_DIM), bf), pltpu.VMEM((HEAD_DIM, NP * PR), bf),
            dma((8,)),
            pltpu.VMEM((ntp, T, depth), jnp.bfloat16),
            pltpu.VMEM((S, C, CHUNK, HEAD_DIM), jnp.bfloat16),
            pltpu.VMEM((S, C, NPP, CHUNK), jnp.float32),
            pltpu.VMEM((S + 1, C, HEAD_DIM, CHUNK), jnp.bfloat16),
            pltpu.VMEM((S + 1, C, 8, CHUNK), jnp.float32),
            pltpu.VMEM((S, C, HEAD_DIM, CHUNK), jnp.bfloat16),
            pltpu.VMEM((S, C, 8, CHUNK), jnp.float32),
            pltpu.VMEM((C, 8, CHUNK), jnp.float32),
            dma((3, C)), dma((3, C)), dma((S,)), dma((S,)),
            dma((S, C)), dma((S, C)), dma((S, C)),
            dma((S, C)), dma((S + 1, C)), dma((S, C)), dma((S + 1, C)),
        ],
        compiler_params=pltpu.CompilerParams(
            collective_id=0, has_side_effects=True, vmem_limit_bytes=60 * 1024 * 1024
        ),
    )(
        tokens, w_query, w_key, w_value, flat, ret_query, ret_key, ret_value,
        wg, bias, jnp.cos(angles), jnp.sin(angles), decay,
    )


def solution(mesh):
    placed = (
        P(("grp", "st"), "tp"),
        P(("grp", "st"), "tp"),
        P(("grp", "st"), "tp"),
        P(("grp", "st"), "tp"),
        P(None, "tp"),
        P(None, "tp"),
        P(None, "tp"),
        P(),
        P("st", None, None),
        P(("grp", "st"), None),
    )

    def run(*args):
        heads = args[4].shape[1] // HEAD_DIM
        wide = 2 <= mesh.shape["st"] <= 8 and mesh.shape["tp"] == 4
        fast = wide and heads == mesh.shape["tp"] and args[7].shape[1] == heads
        return jax.shard_map(
            fast_body if fast else body,
            mesh=mesh, in_specs=placed, out_specs=P(("grp", "st"), "tp"), check_vma=False,
        )(*args)

    return run
```

```python
import functools

import jax
import jax.numpy as jnp
from jax import lax
from jax.experimental import pallas as pl
from jax.experimental.pallas import tpu as pltpu
import numpy as np
from jax.sharding import PartitionSpec as P

RET_DIM = 256
HEAD_DIM = 512
BLOCK = 64
NPB = 4
SEQ_LEN = 256


ROTARY_BASE = 10000.0
NORM_EPS = 1e-05


def rotate(values, positions):
    halfway = values.shape[-1] // 2
    inverse = ROTARY_BASE ** (-jnp.arange(halfway, dtype=jnp.float32) / halfway)
    angles = positions.astype(jnp.float32)[:, None, None] * inverse
    cosines, sines = (jnp.cos(angles), jnp.sin(angles))
    leading, trailing = (values[..., :halfway], values[..., halfway:])
    return jnp.concatenate(
        [leading * cosines - trailing * sines, leading * sines + trailing * cosines], axis=-1
    )


def retain(query_rows, key_rows, value_rows, head_start):
    token_count = query_rows.shape[0]
    groups = query_rows.shape[1] // RET_DIM
    layout = (token_count // SEQ_LEN, SEQ_LEN, groups, RET_DIM)
    places = jnp.arange(SEQ_LEN, dtype=jnp.int32)
    rot_query = rotate(query_rows.reshape(layout).astype(jnp.float32), places).astype(jnp.bfloat16)
    rot_key = (
        rotate(key_rows.reshape(layout).astype(jnp.float32), places) * RET_DIM ** (-0.5)
    ).astype(jnp.bfloat16)
    head_number = (head_start + jnp.arange(groups, dtype=jnp.int32)).astype(jnp.float32)
    log_gamma = jnp.log1p(-jnp.exp2(-5.0 - head_number))
    offsets = (places[:, None] - places[None, :]).astype(jnp.float32)
    decays = jnp.where(
        offsets[None] >= 0.0,
        jnp.exp(log_gamma[:, None, None] * jnp.maximum(offsets, 0.0)[None]),
        0.0,
    )
    scores = jnp.einsum("sigd,sjgd->sgij", rot_query, rot_key, preferred_element_type=jnp.float32)
    weights = (scores * decays[None]).astype(jnp.bfloat16)
    output = jnp.einsum(
        "sgij,sjge->sige", weights, value_rows.reshape(layout), preferred_element_type=jnp.float32
    )
    centred = output - jnp.mean(output, -1, keepdims=True)
    normed = centred * lax.rsqrt(jnp.mean(centred * centred, -1, keepdims=True) + NORM_EPS)
    return normed.astype(jnp.bfloat16).reshape(token_count, groups, RET_DIM)


def partial_attend(query_block, kv_rows, head_width):
    leading = kv_rows.shape[:-2]
    groups = query_block.shape[-2]
    split_shape = leading + (kv_rows.shape[-2], groups, HEAD_DIM)
    key_part = kv_rows[..., :head_width].reshape(split_shape)
    value_part = kv_rows[..., head_width:].reshape(split_shape)
    scores = jnp.einsum(
        "...tgd,...rgd->...gtr", query_block, key_part, preferred_element_type=jnp.float32
    ) * HEAD_DIM ** (-0.5)
    highest = jnp.max(scores, -1)
    exponent = jnp.exp(scores - highest[..., None])
    totals = jnp.sum(exponent, -1)
    weighted = jnp.einsum(
        "...gtr,...rgd->...tgd",
        exponent.astype(jnp.bfloat16),
        value_part,
        preferred_element_type=jnp.float32,
    )
    return (
        weighted.astype(jnp.bfloat16).reshape(leading + (query_block.shape[-3], head_width)),
        highest,
        totals,
    )


def combine(weighted, highest, totals, gate_vals):
    block_count, per_block, span_len, head_width = weighted.shape
    groups = highest.shape[2]
    overall = jnp.max(highest, 1, keepdims=True)
    scales = jnp.exp(highest - overall)
    denominator = jnp.sum(scales * totals, 1)
    pieces = (
        lax.optimization_barrier(weighted)
        .reshape(block_count, per_block, span_len, groups, head_width // groups)
        .astype(jnp.float32)
    )
    numerator = jnp.sum(jnp.transpose(scales, (0, 1, 3, 2))[..., None] * pieces, 1)
    gate_cols = gate_vals.reshape(block_count, span_len, groups)[..., None]
    result = gate_cols * numerator / jnp.transpose(denominator, (0, 2, 1))[..., None]
    return result.astype(jnp.bfloat16).reshape(block_count * span_len, groups, head_width // groups)


def body(
    tokens, ret_query, ret_key, ret_value, w_query, w_key, w_value, w_gate, store, passage_ids
):
    owners = lax.axis_size("st")
    head_rank = lax.axis_index("tp")
    groups = w_query.shape[1] // HEAD_DIM
    head_width = groups * HEAD_DIM
    token_count = tokens.shape[0]
    block_count = token_count // BLOCK
    retained = retain(ret_query, ret_key, ret_value, head_rank * groups)
    shard_cols = lax.all_gather(tokens, "tp", axis=1, tiled=True)
    query_sum = jnp.dot(shard_cols, w_query, preferred_element_type=jnp.float32)
    gate_sum = jnp.dot(shard_cols, w_gate, preferred_element_type=jnp.float32)
    gate_vals = jax.nn.sigmoid(lax.dynamic_slice_in_dim(gate_sum, head_rank * groups, groups, 1))
    query_blocks = query_sum.astype(jnp.bfloat16).reshape(block_count, BLOCK, groups, HEAD_DIM)
    kv_own = jnp.concatenate(
        [
            jnp.dot(store, w_key, preferred_element_type=jnp.float32).astype(jnp.bfloat16),
            jnp.dot(store, w_value, preferred_element_type=jnp.float32).astype(jnp.bfloat16),
        ],
        axis=-1,
    )
    flat_ids = passage_ids.reshape(-1)
    requests = flat_ids.shape[0]
    capacity = max(2, 2 * requests // owners)
    owner_of = flat_ids // store.shape[0]
    within = flat_ids % store.shape[0]
    hit_table = (owner_of[:, None] == jnp.arange(owners, dtype=jnp.int32)[None, :]).astype(
        jnp.int32
    )
    earlier = (
        jnp.arange(requests, dtype=jnp.int32)[:, None]
        > jnp.arange(requests, dtype=jnp.int32)[None, :]
    ).astype(jnp.int32)
    slot_of = jnp.sum(jnp.dot(earlier, hit_table) * hit_table, 1)
    placed = (
        hit_table[:, :, None]
        * (slot_of[:, None] == jnp.arange(capacity, dtype=jnp.int32)[None, :]).astype(jnp.int32)[
            :, None, :
        ]
    )
    wanted = jnp.sum(placed * within[:, None, None], 0)
    fetch_at = owner_of * capacity + slot_of
    block_of = jnp.sum(placed * (jnp.arange(requests, dtype=jnp.int32) // NPB)[:, None, None], 0)
    outgoing = jnp.take(query_blocks, block_of, axis=0)
    incoming = lax.all_to_all(outgoing, "st", split_axis=0, concat_axis=0, tiled=True)
    indices = lax.all_to_all(wanted, "st", split_axis=0, concat_axis=0, tiled=True)
    weighted_here, highest_here, totals_here = partial_attend(
        incoming, jnp.take(kv_own, indices, axis=0), head_width
    )
    back_values = lax.all_to_all(weighted_here, "st", split_axis=0, concat_axis=0, tiled=True)
    returned = (
        back_values,
        lax.all_to_all(highest_here, "st", split_axis=0, concat_axis=0, tiled=True),
        lax.all_to_all(totals_here, "st", split_axis=0, concat_axis=0, tiled=True),
    )
    weighted = jnp.take(
        returned[0].reshape((owners * capacity,) + returned[0].shape[2:]), fetch_at, axis=0
    )
    weighted = weighted.reshape(block_count, NPB, BLOCK, head_width)
    highest = jnp.take(
        returned[1].reshape((owners * capacity,) + returned[1].shape[2:]), fetch_at, axis=0
    )
    highest = highest.reshape(block_count, NPB, groups, BLOCK)
    totals = jnp.take(
        returned[2].reshape((owners * capacity,) + returned[2].shape[2:]), fetch_at, axis=0
    )
    totals = totals.reshape(block_count, NPB, groups, BLOCK)
    retrieved = combine(weighted, highest, totals, gate_vals)
    return jnp.concatenate([retained, retrieved], -1).reshape(
        token_count, groups * (RET_DIM + HEAD_DIM)
    )

MESH = pl.DeviceIdType.MESH
NONE = -1e30
CHUNK = 128
LAG = 0
HOP = 1
HALF = HEAD_DIM // 2


def mixer_kernel(
    S, C, NP, PR,
    tok_h, wq_h, wk_h, wv_h, store_h, rq_h, rk_h, rv_h, wg, bias, cosines, sines, out,
    tok, wq, wk, wv, store, rq, rk, rv, keys, vals, lsem,
    xg, qbuf, bin_, rin, sin_, rout, sout, gates,
    xsend, xrecv, bsend, brecv, qsl, qsr, qrecv, rsend, rrecv, ssend, srecv,
):
    s = lax.axis_index("st")
    tp = lax.axis_index("tp")
    core = lax.rem(tp, 2)
    sib = tp + 1 - 2 * core
    opp = lax.rem(tp + 2, 4)
    diag = lax.rem(sib + 2, 4)
    CH = qbuf.shape[3]
    depth = tok.shape[1]
    scale = HEAD_DIM ** (-0.5)
    loads = [
        pltpu.make_async_copy(a, b, lsem.at[n])
        for n, (a, b) in enumerate((
            (tok_h, tok), (store_h, store), (wk_h, wk), (wq_h, wq), (wv_h, wv),
            (rq_h, rq), (rk_h, rk), (rv_h, rv),
        ))
    ]
    for load in loads:
        load.start()

    barrier = pltpu.get_barrier_semaphore()
    for peer in (sib, opp):
        pl.semaphore_signal(barrier, inc=1, device_id={"tp": peer}, device_id_type=MESH)
    for k in range(1, S):
        pl.semaphore_signal(
            barrier, inc=1, device_id={"st": lax.rem(s + k, S)}, device_id_type=MESH
        )
    pl.semaphore_wait(barrier, S + 1)
    loads[0].wait()

    def rows(i):
        return pl.ds(pl.multiple_of(i * CH, CH), CH)

    def xcopy(kind, i):
        src = tok.at[rows(i)] if kind < 2 else xg.at[opp, rows(i)]
        slot = tp if kind < 2 else opp
        return pltpu.make_async_remote_copy(
            src_ref=src, dst_ref=xg.at[slot, rows(i)],
            send_sem=xsend.at[kind, i], recv_sem=xrecv.at[kind, i],
            device_id={"tp": opp if kind == 0 else sib}, device_id_type=MESH,
        )

    def bcopy(k):
        o = lax.rem(s + k, S)
        return pltpu.make_async_remote_copy(
            src_ref=bias.at[o], dst_ref=bin_.at[s],
            send_sem=bsend.at[k], recv_sem=brecv.at[k],
            device_id={"st": o}, device_id_type=MESH,
        )

    for i in range(C):
        xcopy(0, i).start()
        xcopy(1, i).start()
    for k in range(1, S):
        bcopy(k).start()
    bin_[s] = bias[s]

    def qcopy(u, i, right, h):
        return pltpu.make_async_remote_copy(
            src_ref=qbuf.at[u, i, h], dst_ref=qbuf.at[u, i, h],
            send_sem=(qsr if right else qsl).at[u, i, h], recv_sem=qrecv.at[u, i, h],
            device_id={"st": s + 1 if right else s - 1}, device_id_type=MESH,
        )

    def rcopy(u, i, left, n):
        slot = u if left else jnp.where(s + 1 == u, S, u)
        at = (i,) if n == 2 else (i, n)
        src, dst = (sout, sin_) if n == 2 else (rout, rin)
        out_sem, in_sem = (ssend, srecv) if n == 2 else (rsend, rrecv)
        return pltpu.make_async_remote_copy(
            src_ref=src.at[(u,) + at], dst_ref=dst.at[(slot,) + at],
            send_sem=out_sem.at[(u,) + at], recv_sem=in_sem.at[(slot,) + at],
            device_id={"st": s - 1 if left else s + 1}, device_id_type=MESH,
        )

    def arrived(data, slot, i, *h):
        buf, out_sem, in_sem = (rin, rsend, rrecv) if data else (sin_, ssend, srecv)
        ref = buf.at[(slot, i) + h]
        pltpu.make_async_remote_copy(
            src_ref=ref, dst_ref=ref,
            send_sem=out_sem.at[(0, i) + h], recv_sem=in_sem.at[(slot, i) + h],
            device_id={"st": lax.rem(s + 1, S)}, device_id_type=MESH,
        ).wait_recv()

    def gate_part(j, part):
        cols = pl.ds(pl.multiple_of(j * depth, depth), depth)
        return lax.dot_general(
            wg[:, cols], part, (((1,), (1,)), ((), ())), preferred_element_type=jnp.float32
        )

    RB = 2 * PR if NP % 2 == 0 else PR

    def key_rows(n, c):
        r = pl.ds(pl.multiple_of(n * RB, RB), RB)
        keys[r] = jnp.dot(
            store[r], wk[...], preferred_element_type=jnp.float32
        ).astype(jnp.bfloat16)
        return c

    def value_rows(n, c):
        r = pl.ds(pl.multiple_of(n * RB, RB), RB)
        vals[:, r] = jnp.dot(
            store[r], wv[...], preferred_element_type=jnp.float32
        ).T.astype(jnp.bfloat16)
        return c

    def turned(ref, r, factor):
        half = RET_DIM // 2
        a = ref[r, :half].astype(jnp.float32)
        b = ref[r, half:].astype(jnp.float32)
        cs, sn = cosines[...], sines[...]
        both = jnp.concatenate([a * cs - b * sn, a * sn + b * cs], -1) * factor
        return both.astype(jnp.bfloat16)

    def retention(n):
        r = pl.ds(pl.multiple_of(n * SEQ_LEN, SEQ_LEN), SEQ_LEN)
        sc = lax.dot_general(
            turned(rq, r, 1.0), turned(rk, r, RET_DIM ** (-0.5)),
            (((1,), (1,)), ((), ())), preferred_element_type=jnp.float32,
        )
        offset = (
            lax.broadcasted_iota(jnp.int32, sc.shape, 0)
            - lax.broadcasted_iota(jnp.int32, sc.shape, 1)
        ).astype(jnp.float32)
        log_gamma = jnp.float32(0.0)
        for h in range(4):
            log_gamma = jnp.where(tp == h, float(np.log1p(-(2.0 ** (-5 - h)))), log_gamma)
        decay = jnp.where(offset >= 0.0, jnp.exp(log_gamma * jnp.maximum(offset, 0.0)), 0.0)
        raw = jnp.dot(
            (sc * decay).astype(jnp.bfloat16), rv[r], preferred_element_type=jnp.float32
        )
        mid = raw - jnp.mean(raw, -1, keepdims=True)
        var = jnp.mean(mid * mid, -1, keepdims=True)
        out[r, :RET_DIM] = (mid * lax.rsqrt(var + NORM_EPS)).astype(jnp.bfloat16)

    def project(i):
        xcopy(0, i).wait_recv()
        xcopy(2, i).start()
        acc = jnp.dot(
            tok[rows(i)], wq[pl.ds(pl.multiple_of(tp * depth, depth), depth)],
            preferred_element_type=jnp.float32,
        )
        gate = gate_part(tp, tok[rows(i)])
        xcopy(1, i).wait_recv()
        for j in (opp, sib, diag):
            if j is diag:
                xcopy(2, i).wait_recv()
            part = xg[j, rows(i)]
            acc += jnp.dot(
                part, wq[pl.ds(pl.multiple_of(j * depth, depth), depth)],
                preferred_element_type=jnp.float32,
            )
            gate += gate_part(j, part)
        gates[i] = jax.nn.sigmoid(gate[:8])
        mixed = acc.astype(jnp.bfloat16)
        for h in range(2):
            qbuf[s, i, h] = mixed[:, h * HALF:(h + 1) * HALF]

    def attend(u, i):
        sc = sum(
            lax.dot_general(
                keys[:, h * HALF:(h + 1) * HALF], qbuf[u, i, h],
                (((1,), (1,)), ((), ())), preferred_element_type=jnp.float32,
            )
            for h in range(2)
        ) * scale
        sc = sc.reshape(NP, PR, CH) + bin_[u, i][:NP][:, None, :]
        top = jnp.max(jnp.max(sc, 0), 0, keepdims=True)
        ex = jnp.exp(sc - top[None])
        tot = jnp.sum(jnp.sum(ex, 0), 0, keepdims=True)
        part = jnp.dot(
            vals[...], ex.reshape(NP * PR, CH).astype(jnp.bfloat16),
            preferred_element_type=jnp.float32,
        )
        for h in range(2):
            rout[u, i, h] = part[h * HALF:(h + 1) * HALF].astype(jnp.bfloat16)
        sout[u, i] = jnp.concatenate(
            [jnp.broadcast_to(top, (4, CH)), jnp.broadcast_to(tot, (4, CH))], 0
        )

    def merge(u, i, slot, send):
        arrived(False, slot, i)
        a, b = sout[u, i], sin_[slot, i]
        ma, ta, mb, tb = a[0:1], a[4:5], b[0:1], b[4:5]
        top = jnp.maximum(ma, mb)
        fa, fb = jnp.exp(ma - top), jnp.exp(mb - top)
        tot = fa * ta + fb * tb
        sout[u, i] = jnp.concatenate(
            [jnp.broadcast_to(top, (4, CH)), jnp.broadcast_to(tot, (4, CH))], 0
        )
        if send:
            send(2)
        for h in range(2):
            arrived(True, slot, i, h)
            mixed = rout[u, i, h].astype(jnp.float32) * fa
            mixed += rin[slot, i, h].astype(jnp.float32) * fb
            rout[u, i, h] = mixed.astype(jnp.bfloat16)
            if send:
                send(h)

    loads[1].wait()
    loads[2].wait()
    lax.fori_loop(0, NP * PR // RB, key_rows, 0)
    loads[3].wait()
    steps = C + 2 * HOP * (S - 1) + LAG
    seqs = tok.shape[0] // SEQ_LEN

    def step(t, carry):
        @pl.when(t < C)
        def _():
            project(t)

            for h in range(2):
                @pl.when(s < S - 1)
                def _():
                    qcopy(s, t, True, h).start()

                @pl.when(s > 0)
                def _():
                    qcopy(s, t, False, h).start()

        @pl.when(t == 0)
        def _():
            loads[4].wait()
            lax.fori_loop(0, NP * PR // RB, value_rows, 0)
            for k in range(1, S):
                bcopy(k).wait_recv()

        def source(u, c):
            k = jnp.abs(s - u)
            i = t - HOP * k

            @pl.when((u != s) & (i >= 0) & (i < C))
            def _():
                for h in range(2):
                    qcopy(u, i, True, h).wait_recv()

                    @pl.when((u < s) & (s < S - 1))
                    def _():
                        qcopy(u, i, True, h).start()

                    @pl.when((u > s) & (s > 0))
                    def _():
                        qcopy(u, i, False, h).start()

            n = i - LAG

            @pl.when((n >= 0) & (n < C))
            def _():
                attend(u, n)

            far = jnp.where(u < s, S - 1 - u, u)
            m = t - HOP * (2 * far - k) - LAG

            @pl.when((u != s) & (m >= 0) & (m < C))
            def _():
                def send(n):
                    @pl.when(u < s)
                    def _():
                        rcopy(u, m, True, n).start()

                    @pl.when(u > s)
                    def _():
                        rcopy(u, m, False, n).start()

                @pl.when(k < far)
                def _():
                    merge(u, m, u, send)

                @pl.when(k == far)
                def _():
                    for n in (2, 0, 1):
                        send(n)

            return c

        lax.fori_loop(0, S, source, 0)

        first = steps - 1 - seqs

        @pl.when(t == first)
        def _():
            for load in loads[5:]:
                load.wait()

        @pl.when((t >= first) & (t < first + seqs))
        def _():
            retention(t - first)

        last = t - 2 * HOP * jnp.maximum(s, S - 1 - s) - LAG

        @pl.when((last >= 0) & (last < C))
        def _():
            @pl.when(s < S - 1)
            def _():
                merge(s, last, s, None)

            @pl.when(s > 0)
            def _():
                merge(s, last, S, None)

            ratio = gates[last, pl.ds(tp, 1)] / sout[s, last][4:5]
            for h in range(2):
                res = rout[s, last, h].astype(jnp.float32) * ratio
                cols = slice(RET_DIM + h * HALF, RET_DIM + (h + 1) * HALF)
                out[rows(last), cols] = res.T.astype(jnp.bfloat16)

        return carry

    lax.fori_loop(0, steps, step, 0)

    for i in range(C):
        for kind in range(3):
            xcopy(kind, i).wait_send()
    for k in range(1, S):
        bcopy(k).wait_send()

    def drain(n, c):
        u, i = n // C, n % C

        @pl.when((u <= s) & (s < S - 1))
        def _():
            for h in range(2):
                qcopy(u, i, True, h).wait_send()

        @pl.when((u >= s) & (s > 0))
        def _():
            for h in range(2):
                qcopy(u, i, False, h).wait_send()

        @pl.when(u < s)
        def _():
            for n in range(3):
                rcopy(u, i, True, n).wait_send()

        @pl.when(u > s)
        def _():
            for n in range(3):
                rcopy(u, i, False, n).wait_send()

        return c

    lax.fori_loop(0, S * C, drain, 0)


def fast_body(
    tokens, ret_query, ret_key, ret_value, w_query, w_key, w_value, w_gate, store, passage_ids
):
    S = lax.axis_size("st")
    ntp = lax.axis_size("tp")
    head = lax.axis_index("tp")
    T, depth = tokens.shape
    NP, PR, D = store.shape
    C = T // CHUNK
    per = CHUNK // BLOCK
    NPP = -(-NP // 8) * 8
    heads = w_gate.shape[1]
    flat = store.reshape(NP * PR, D)
    wg = jnp.pad(w_gate.T, ((0, -heads % 16), (0, 0)))
    half = RET_DIM // 2
    inverse = ROTARY_BASE ** (-np.arange(half, dtype=np.float32) / half)
    angles = np.arange(SEQ_LEN, dtype=np.float32)[:, None] * inverse.astype(np.float32)
    names = jnp.arange(S * NP, dtype=jnp.int32)
    counts = jnp.sum((passage_ids[:, :, None] == names).astype(jnp.float32), 1)
    bias = jnp.where(counts > 0, jnp.log(jnp.maximum(counts, 1.0)), NONE)
    bias = bias.reshape(C, per, S, NP).transpose(2, 0, 3, 1)
    bias = jnp.pad(bias, ((0, 0), (0, 0), (0, NPP - NP), (0, 0)), constant_values=NONE)
    bias = jnp.repeat(bias, BLOCK, axis=3)

    vm = pl.BlockSpec(memory_space=pltpu.VMEM)
    hbm = pl.BlockSpec(memory_space=pl.ANY)
    bf = jnp.bfloat16
    dma = pltpu.SemaphoreType.DMA
    return pl.pallas_call(
        functools.partial(mixer_kernel, S, C, NP, PR),
        out_shape=jax.ShapeDtypeStruct((T, RET_DIM + HEAD_DIM), jnp.bfloat16),
        in_specs=[hbm] * 8 + [vm] * 4,
        out_specs=vm,
        scratch_shapes=[
            pltpu.VMEM((T, depth), bf),
            pltpu.VMEM(w_query.shape, bf), pltpu.VMEM(w_key.shape, bf),
            pltpu.VMEM(w_value.shape, bf), pltpu.VMEM(flat.shape, bf),
            pltpu.VMEM((T, RET_DIM), bf), pltpu.VMEM((T, RET_DIM), bf),
            pltpu.VMEM((T, RET_DIM), bf),
            pltpu.VMEM((NP * PR, HEAD_DIM), bf), pltpu.VMEM((HEAD_DIM, NP * PR), bf),
            dma((8,)),
            pltpu.VMEM((ntp, T, depth), jnp.bfloat16),
            pltpu.VMEM((S, C, 2, CHUNK, HALF), jnp.bfloat16),
            pltpu.VMEM((S, C, NPP, CHUNK), jnp.float32),
            pltpu.VMEM((S + 1, C, 2, HALF, CHUNK), jnp.bfloat16),
            pltpu.VMEM((S + 1, C, 8, CHUNK), jnp.float32),
            pltpu.VMEM((S, C, 2, HALF, CHUNK), jnp.bfloat16),
            pltpu.VMEM((S, C, 8, CHUNK), jnp.float32),
            pltpu.VMEM((C, 8, CHUNK), jnp.float32),
            dma((3, C)), dma((3, C)), dma((S,)), dma((S,)),
            dma((S, C, 2)), dma((S, C, 2)), dma((S, C, 2)),
            dma((S, C, 2)), dma((S + 1, C, 2)), dma((S, C)), dma((S + 1, C)),
        ],
        compiler_params=pltpu.CompilerParams(
            collective_id=0, has_side_effects=True, vmem_limit_bytes=60 * 1024 * 1024
        ),
    )(
        tokens, w_query, w_key, w_value, flat, ret_query, ret_key, ret_value,
        wg, bias, jnp.asarray(np.cos(angles), jnp.float32), jnp.asarray(np.sin(angles), jnp.float32),
    )


def solution(mesh):
    placed = (
        P(("grp", "st"), "tp"),
        P(("grp", "st"), "tp"),
        P(("grp", "st"), "tp"),
        P(("grp", "st"), "tp"),
        P(None, "tp"),
        P(None, "tp"),
        P(None, "tp"),
        P(),
        P("st", None, None),
        P(("grp", "st"), None),
    )

    def run(*args):
        heads = args[4].shape[1] // HEAD_DIM
        wide = 2 <= mesh.shape["st"] <= 8 and mesh.shape["tp"] == 4
        fast = wide and heads == mesh.shape["tp"] and args[7].shape[1] == heads
        return jax.shard_map(
            fast_body if fast else body,
            mesh=mesh, in_specs=placed, out_specs=P(("grp", "st"), "tp"), check_vma=False,
        )(*args)

    return run
```
